32 devices in a mesh: sp: 4 (over x, core), dp: 8 (over z, y).
Axes of the slice: x: 2, y: 2, z: 4, core: 2. Of those that a mesh axis runs over, the one named last changes fastest.
Arguments:
- content_features_raw: bfloat16 [8, 512, 3072], P('dp', 'sp'), may hold values from -6 to 6
- memory_entering_matrix: bfloat16 [8, 512, 2048], P('dp', 'sp'), may hold values from -6 to 6
- memory_leaving_matrix: bfloat16 [8, 512, 2048], P('dp', 'sp'), may hold values from -6 to 6
- feature_switch_signal: bfloat16 [8, 512, 3072], P('dp', 'sp'), may hold values from -6 to 6
- ahead_increment_raw: float32 [8, 512, 48], P('dp', 'sp'), may hold values from -5 to 5
- reverse_increment_raw: float32 [8, 512, 48], P('dp', 'sp'), may hold values from -5 to 5
- additional_fading: float32 [8, 512, 48], P('dp', 'sp'), as said below
- content_filter_weights: bfloat16 [4, 3072], P(None, 'sp'), may hold values from -3 to 3
- entering_filter_weights: bfloat16 [4, 2048], P(None, 'sp'), may hold values from -3 to 3
- leaving_filter_weights: bfloat16 [4, 2048], P(None, 'sp'), may hold values from -3 to 3
- increment_offset_lanes: float32 [2, 48], P(None, 'sp'), may hold values from -0.5 to 0.5
- fading_speed_exponents: float32 [2, 48], P(None, 'sp'), as said below
- result_scaling_factor: bfloat16 [3072], replicated, may hold values from 0.099609375 to 1.8984375
Outputs:
- out: bfloat16 [8, 512, 3072], P('dp', 'sp')
The draws below stay inside these ranges and needn't reach their ends.
Inputs may be any that keep to these rules, and one draw needn't show every extreme that they name: Each head's row has a rate exp(fading_speed_exponents) between 0.3 / 4096 and 0.05. `additional_fading`: zero at most positions; elsewhere between log(0.5) and log(0.8).
All inputs are finite; a program needn't handle non-finite values.
Results may differ from the reference program's by a relative error of at most 0.0051.
Values may be sent and summed in bfloat16 or wider, within the bound.
No kernel may reach another device: no remote copies, remote signals or barrier semaphores. Data moves between devices by JAX's collectives and lax.ppermute only.
A program may use at most 64 MiB of HBM per device.

```python
import math
import jax
import jax.numpy as jnp
from jax import lax

ATTENTION_LANES = 48
HEAD_DIM = 64
GROUPS = 16
STATE = 128
TAPS = 4
BLK = 128
TOK_DEV = 128
SEGMENTS = 8
SEG_LEN = 512
SEQ_LEN = 4096
D_SSM = 3072


def draw_fading_speed_exponents(key, part):
    first_key, second_key, third_key = jax.random.split(key, 3)
    share = 0.5
    slow_pick = jax.random.uniform(first_key, (2, ATTENTION_LANES), jnp.float32) < share
    slow_low = math.log(0.3 / SEQ_LEN)
    slow_high = math.log(min(2.0 / SEG_LEN, 0.015))
    slow_rate = jax.random.uniform(second_key, (2, ATTENTION_LANES), jnp.float32, slow_low, slow_high)
    fast_rate = jax.random.uniform(third_key, (2, ATTENTION_LANES), jnp.float32, math.log(0.015), math.log(0.05))
    return jnp.where(slow_pick, slow_rate, fast_rate).astype(jnp.float32)


def step_rates(key, salt):
    folded = jax.random.fold_in(key, salt)
    first_key, second_key = jax.random.split(folded)
    block_count = SEQ_LEN // TOK_DEV
    noise_draw = jnp.clip(jax.random.normal(first_key, (block_count, TOK_DEV, ATTENTION_LANES), jnp.float32), -3.0, 3.0)
    offset = jax.random.uniform(second_key, (block_count, 1, ATTENTION_LANES), jnp.float32, -1.2, 1.2)
    return (noise_draw + offset).reshape(SEGMENTS, SEG_LEN, ATTENTION_LANES).astype(jnp.float32)


def draw_ahead_increment_raw(key, part):
    return step_rates(key, 11)


def draw_reverse_increment_raw(key, part):
    return step_rates(key, 23)


def draw_additional_fading(key, part):
    first_key, second_key = jax.random.split(key)
    struck = jax.random.uniform(first_key, (SEGMENTS, SEG_LEN, ATTENTION_LANES), jnp.float32) < 3.0 / SEQ_LEN
    loss_log = jnp.log(jax.random.uniform(second_key, (SEGMENTS, SEG_LEN, ATTENTION_LANES), jnp.float32, 0.5, 0.8))
    return jnp.where(struck, loss_log, 0.0).astype(jnp.float32)


def levels(rng, extent, cuts, low, largest):
    def one(position, shards_of):
        steps = jax.random.uniform(jax.random.fold_in(jax.random.fold_in(rng, 6), position), (shards_of,), jnp.float32, low / len(cuts), largest / len(cuts))
        return jnp.repeat(jnp.exp(steps), extent[position] // shards_of).reshape((-1,) + (1,) * (len(extent) - position - 1))

    level = one(*cuts[0])
    for cut in cuts[1:]:
        level = level * one(*cut)
    return level


def gaussian(stream_key, extent, spread, limit, shards=(), kind=jnp.bfloat16):
    values = jax.random.normal(stream_key, extent, jnp.float32) * spread
    if len(shards) > 0:
        values = levels(stream_key, extent, shards, -0.22, 0.18) * values
    return jnp.clip(values, min=-limit, max=limit).astype(kind)


def setup_inputs(seed: int = 0) -> dict:
    streams_of = jax.random.split(jax.random.key(seed), 14)
    content_features_raw = gaussian(streams_of[0], (SEGMENTS, SEG_LEN, D_SSM), 1.0, 6.0, ((0, 8), (1, 4)))
    memory_entering_matrix = gaussian(streams_of[1], (SEGMENTS, SEG_LEN, GROUPS * STATE), 1.0, 6.0, ((0, 8), (1, 4)))
    memory_leaving_matrix = gaussian(streams_of[2], (SEGMENTS, SEG_LEN, GROUPS * STATE), 1.0, 6.0, ((0, 8), (1, 4)))
    feature_switch_signal = gaussian(streams_of[3], (SEGMENTS, SEG_LEN, D_SSM), 1.0, 6.0, ((0, 8), (1, 4)))
    ahead_increment_raw = draw_ahead_increment_raw(jax.random.fold_in(streams_of[13], 71), 0)
    reverse_increment_raw = draw_reverse_increment_raw(jax.random.fold_in(streams_of[13], 71), 0)
    additional_fading = draw_additional_fading(jax.random.fold_in(streams_of[13], 71), 0)
    content_filter_weights = gaussian(streams_of[7], (TAPS, D_SSM), TAPS ** -0.5, 3.0, ((1, 4),))
    entering_filter_weights = gaussian(streams_of[8], (TAPS, GROUPS * STATE), TAPS ** -0.5, 3.0, ((1, 4),))
    leaving_filter_weights = gaussian(streams_of[9], (TAPS, GROUPS * STATE), TAPS ** -0.5, 3.0, ((1, 4),))
    increment_offset_lanes = jnp.clip(jax.random.uniform(streams_of[10], (2, ATTENTION_LANES), jnp.float32, -0.5, 0.5) * levels(streams_of[10], (2, ATTENTION_LANES), ((1, 4),), -0.4, 0.0), -0.5, 0.5)
    fading_speed_exponents = draw_fading_speed_exponents(jax.random.fold_in(streams_of[13], 71), 0)
    result_scaling_factor = jnp.clip(1.0 + 0.18 * jax.random.normal(streams_of[12], (D_SSM,), jnp.float32), 0.099609375, 1.8984375).astype(jnp.bfloat16)
    return {"content_features_raw": content_features_raw, "memory_entering_matrix": memory_entering_matrix, "memory_leaving_matrix": memory_leaving_matrix, "feature_switch_signal": feature_switch_signal, "ahead_increment_raw": ahead_increment_raw, "reverse_increment_raw": reverse_increment_raw, "additional_fading": additional_fading, "content_filter_weights": content_filter_weights, "entering_filter_weights": entering_filter_weights, "leaving_filter_weights": leaving_filter_weights, "increment_offset_lanes": increment_offset_lanes, "fading_speed_exponents": fading_speed_exponents, "result_scaling_factor": result_scaling_factor}


def conv_silu(padded, weight, length):
    total_sum = padded[0:length].astype(jnp.float32) * weight[0].astype(jnp.float32)
    for lag_step in range(1, weight.shape[0]):
        total_sum = total_sum + padded[lag_step:lag_step + length].astype(jnp.float32) * weight[lag_step].astype(jnp.float32)
    return jax.nn.silu(total_sum).astype(jnp.bfloat16)

def direction(x_conv, b_conv, c_conv, rate, log_decay):
    overall_position_count = x_conv.shape[0]
    heads_within_group = rate.shape[1]
    block_count = overall_position_count // BLK
    x_blocks = x_conv.reshape(block_count, BLK, heads_within_group, HEAD_DIM)
    b_blocks = b_conv.reshape(block_count, BLK, STATE)
    c_blocks = c_conv.reshape(block_count, BLK, STATE)
    rate_blocks = rate.reshape(block_count, BLK, heads_within_group)
    log_blocks = log_decay.reshape(block_count, BLK, heads_within_group)
    lower_mask = jnp.tril(jnp.ones((BLK, BLK), bool))[:, :, None]

    def step(state, pieces):
        x_block, b_block, c_block, rate_block, log_block = pieces
        cum_log = jnp.cumsum(log_block, axis=0)
        scores = jnp.dot(c_block, b_block.T, preferred_element_type=jnp.float32)
        log_gaps = jnp.where(lower_mask, cum_log[:, None, :] - cum_log[None, :, :], -jnp.inf)
        weights = (scores[:, :, None] * jnp.exp(log_gaps) * rate_block[None, :, :]).astype(jnp.bfloat16)
        local_part = jnp.einsum('lsh,shp->lhp', weights.astype(jnp.float32), x_block.astype(jnp.float32))
        carried_part = jnp.einsum('ln,hpn->lhp', c_block.astype(jnp.float32), state, precision=lax.Precision.HIGHEST) * jnp.exp(cum_log)[:, :, None]
        block_log = cum_log[-1]
        scaled = (x_block.astype(jnp.float32) * (rate_block * jnp.exp(block_log[None, :] - cum_log))[:, :, None]).astype(jnp.bfloat16)
        update = jnp.einsum('shp,sn->hpn', scaled.astype(jnp.float32), b_block.astype(jnp.float32))
        new_state = state * jnp.exp(block_log)[:, None, None] + update
        return (new_state, local_part + carried_part)
    initial = jnp.zeros((heads_within_group, HEAD_DIM, STATE), jnp.float32)
    _, outputs = lax.scan(step, initial, (x_blocks, b_blocks, c_blocks, rate_blocks, log_blocks))
    return outputs.reshape(overall_position_count, heads_within_group * HEAD_DIM)

def reference(content_features_raw, memory_entering_matrix, memory_leaving_matrix, feature_switch_signal, ahead_increment_raw, reverse_increment_raw, additional_fading, content_filter_weights, entering_filter_weights, leaving_filter_weights, increment_offset_lanes, fading_speed_exponents, result_scaling_factor):
    overall_position_count = SEGMENTS * SEG_LEN
    width = ATTENTION_LANES * HEAD_DIM
    heads_within_group = ATTENTION_LANES // GROUPS
    group_width = heads_within_group * HEAD_DIM
    x_flat = content_features_raw.reshape(overall_position_count, width)
    b_flat = memory_entering_matrix.reshape(overall_position_count, GROUPS * STATE)
    c_flat = memory_leaving_matrix.reshape(overall_position_count, GROUPS * STATE)
    z_flat = feature_switch_signal.reshape(overall_position_count, width)
    fwd_flat = ahead_increment_raw.reshape(overall_position_count, ATTENTION_LANES)
    bwd_flat = reverse_increment_raw.reshape(overall_position_count, ATTENTION_LANES)
    additional_fading_flat_array = additional_fading.reshape(overall_position_count, ATTENTION_LANES)

    def one_group(group):
        col_x = (group * group_width).astype(jnp.int32)
        col_b = (group * STATE).astype(jnp.int32)
        column_per_head = (group * heads_within_group).astype(jnp.int32)
        x_part = lax.dynamic_slice_in_dim(x_flat, col_x, group_width, 1)
        b_part = lax.dynamic_slice_in_dim(b_flat, col_b, STATE, 1)
        c_part = lax.dynamic_slice_in_dim(c_flat, col_b, STATE, 1)
        z_part = lax.dynamic_slice_in_dim(z_flat, col_x, group_width, 1)
        pad_rows = ((2, TAPS - 3), (0, 0))
        x_conv = conv_silu(jnp.pad(x_part, pad_rows), lax.dynamic_slice_in_dim(content_filter_weights, col_x, group_width, 1), overall_position_count)
        b_conv = conv_silu(jnp.pad(b_part, pad_rows), lax.dynamic_slice_in_dim(entering_filter_weights, col_b, STATE, 1), overall_position_count)
        c_conv = conv_silu(jnp.pad(c_part, pad_rows), lax.dynamic_slice_in_dim(leaving_filter_weights, col_b, STATE, 1), overall_position_count)
        bias_part = lax.dynamic_slice_in_dim(increment_offset_lanes, column_per_head, heads_within_group, 1)
        decay_log_piece = lax.dynamic_slice_in_dim(fading_speed_exponents, column_per_head, heads_within_group, 1)
        spike_piece = lax.dynamic_slice_in_dim(additional_fading_flat_array, column_per_head, heads_within_group, 1)
        forward_step_rate = jax.nn.softplus(lax.dynamic_slice_in_dim(fwd_flat, column_per_head, heads_within_group, 1) + bias_part[0])
        backward_step_rate = jax.nn.softplus(lax.dynamic_slice_in_dim(bwd_flat, column_per_head, heads_within_group, 1) + bias_part[1])
        forward_log_decay = -jnp.exp(decay_log_piece[0]) * forward_step_rate + spike_piece
        backward_log_decay = -jnp.exp(decay_log_piece[1]) * backward_step_rate + spike_piece
        y_fwd = direction(x_conv, b_conv, c_conv, forward_step_rate, forward_log_decay)
        y_bwd = direction(x_conv[::-1], b_conv[::-1], c_conv[::-1], backward_step_rate[::-1], backward_log_decay[::-1])[::-1]
        mixed = (y_fwd + y_bwd).astype(jnp.bfloat16)
        gated = mixed.astype(jnp.float32) * jax.nn.silu(z_part.astype(jnp.float32))
        by_head = gated.reshape(overall_position_count, heads_within_group, HEAD_DIM)
        normed = by_head * lax.rsqrt(lax.optimization_barrier(jnp.mean(by_head * by_head, axis=-1, keepdims=True)) + 1e-06)
        gain_part = lax.dynamic_slice_in_dim(result_scaling_factor, col_x, group_width, 0).astype(jnp.float32)
        return (normed.reshape(overall_position_count, group_width) * gain_part).astype(jnp.bfloat16)
    results = lax.map(one_group, jnp.arange(GROUPS, dtype=jnp.int32))
    return jnp.transpose(results, (1, 0, 2)).reshape(SEGMENTS, SEG_LEN, width)
```

```python
import jax
import jax.numpy as jnp
from jax import lax
from jax.experimental import pallas as pl
from jax.experimental.pallas import tpu as pltpu
from jax.sharding import PartitionSpec as P

HEAD_DIM = 64
STATE = 128
BLK = 128
HIGH = lax.Precision.HIGHEST
f32 = jnp.float32
bf16 = jnp.bfloat16
ALL = ("dp", "sp")
STEP_HEADS = 6
SLOT = 8
RF, RB, CF, CB, FF, FB, EF, EB = range(8)


def iota(shape, dim):
    return lax.broadcasted_iota(jnp.int32, shape, dim)


def rates_kernel(ahead, back, fade, params, cols, rows, totals):
    steps = cols.shape[0]
    spread = fade[0]
    tri = iota((BLK, BLK), 0) - iota((BLK, BLK), 1)

    def one(raw, d, mask):
        rate = jax.nn.softplus(raw + params[d : d + 1, :])
        log = -jnp.exp(params[2 + d : 3 + d, :]) * rate + spread
        cum = jnp.dot(mask.astype(f32), log, precision=HIGH, preferred_element_type=f32)
        return rate, cum

    rate_f, cum_f = one(ahead[0], 0, tri >= 0)
    rate_b, cum_b = one(back[0], 1, tri <= 0)
    tot_f, tot_b = cum_f[BLK - 1 :], cum_b[:1]
    parts = (
        rate_f,
        rate_b,
        cum_f,
        cum_b,
        rate_f * jnp.exp(tot_f - cum_f),
        rate_b * jnp.exp(tot_b - cum_b),
        jnp.exp(cum_f),
        jnp.exp(cum_b),
    )
    gap = jnp.zeros((BLK, SLOT - STEP_HEADS), f32)
    rest = jnp.zeros((BLK, 128 - SLOT * len(parts)), f32)
    for g in range(steps):
        at = slice(g * STEP_HEADS, (g + 1) * STEP_HEADS)
        pieces = []
        for part in parts:
            pieces += [part[:, at], gap]
        packed = jnp.concatenate(pieces + [rest], axis=1)
        cols[g] = packed
        rows[g] = packed.T[: 4 * SLOT]
    totals[0:1] = tot_f
    totals[1:2] = tot_b


def expand(cols, which, width):
    pick = iota((128, width), 0) == which * SLOT + iota((128, width), 1) // HEAD_DIM
    return jnp.dot(cols, pick.astype(f32), precision=HIGH, preferred_element_type=f32)


def conv(ref, halo, taps):
    edge = halo[...].astype(f32)
    full = jnp.concatenate([edge[:8], ref[0].astype(f32), edge[8:]], axis=0)
    total = full[6 : 6 + BLK] * taps[0:1]
    for k in range(1, taps.shape[0]):
        total = total + full[6 + k : 6 + k + BLK] * taps[k : k + 1]
    return jax.nn.silu(total).astype(bf16)


def state_kernel(x, b, c, xh, bh, ch, xt, bt, ct, cols, xo, bo, co, uf, ub):
    xc, bc = conv(x, xh, xt), conv(b, bh, bt)
    xo[...] = xc
    bo[...] = bc
    co[...] = conv(c, ch, ct)
    width = xc.shape[1]
    half = width // 2
    packed = cols[0]
    xf = xc.astype(f32)
    for which, out in ((FF, uf), (FB, ub)):
        scaled = (xf * expand(packed, which, width)).astype(bf16)
        both = lax.dot_general(
            scaled, bc, (((0,), (0,)), ((), ())), preferred_element_type=f32
        )
        out[:half] = both[:half, :STATE].astype(bf16)
        out[half:] = both[half:, STATE:].astype(bf16)


def block_kernel(x, b, c, cols, rows, out):
    packed, across = cols[0], rows[0]
    ahead = iota((BLK, BLK), 1) - iota((BLK, BLK), 0)
    lower, upper = ahead < 0, ahead > 0
    lane = iota((BLK, 128), 1)
    scores = [
        lax.dot_general(
            c[:, i * STATE : (i + 1) * STATE],
            b[:, i * STATE : (i + 1) * STATE],
            (((1,), (1,)), ((), ())),
            preferred_element_type=f32,
        )
        for i in range(2)
    ]

    def head(j, pair):
        def col(a):
            return packed[:, a * SLOT + j : a * SLOT + j + 1]

        def row(a):
            return across[a * SLOT + j : a * SLOT + j + 1]

        gaps = jnp.where(lower, col(CF) - row(CF), col(CB) - row(CB))
        rate = jnp.where(lower, row(RF), jnp.where(upper, row(RB), row(RF) + row(RB)))
        weights = (scores[j * 2 // STEP_HEADS] * jnp.exp(gaps) * rate).astype(bf16)
        return jnp.dot(weights, pair, preferred_element_type=f32)

    for k in range(STEP_HEADS // 2):
        at = slice(k * 128, (k + 1) * 128)
        pair = x[:, at]
        out[:, at] = jnp.where(lane < HEAD_DIM, head(2 * k, pair), head(2 * k + 1, pair))


def finish_kernel(local, c, cols, sf, sb, gate, gain, out):
    packed = cols[0]
    width = local.shape[1]
    first = iota((BLK, width), 1) < width // 2
    y = local[...]
    for which, state in ((EF, sf), (EB, sb)):
        by_group = [
            lax.dot_general(
                c[:, i * STATE : (i + 1) * STATE],
                state[...],
                (((1,), (1,)), ((), ())),
                preferred_element_type=f32,
            )
            for i in range(2)
        ]
        y = y + jnp.where(first, by_group[0], by_group[1]) * expand(packed, which, width)
    gated = y.astype(bf16).astype(f32) * jax.nn.silu(gate[0].astype(f32))
    same = iota((width, width), 0) // HEAD_DIM == iota((width, width), 1) // HEAD_DIM
    mean = jnp.dot(
        gated * gated,
        jnp.where(same, 1.0 / HEAD_DIM, 0.0),
        precision=HIGH,
        preferred_element_type=f32,
    )
    out[0] = (gated * lax.rsqrt(mean + 1e-6) * gain[...].astype(f32)).astype(bf16)


def scan_kernel(uf, ub, decay, of, ob):
    count = uf.shape[0]
    state = jnp.zeros(uf.shape[1:], f32)
    for p in range(count):
        of[p] = state.astype(bf16)
        state = state * decay[0][:, p : p + 1] + uf[p].astype(f32)
    state = jnp.zeros(uf.shape[1:], f32)
    for p in reversed(range(count)):
        ob[p] = state.astype(bf16)
        state = state * decay[1][:, p : p + 1] + ub[p].astype(f32)


def scan_plain(u, decay, reverse):
    def step(state, piece):
        update, factor = piece
        return state * factor[:, None] + update.astype(f32), state.astype(bf16)

    return lax.scan(step, jnp.zeros(u.shape[1:], f32), (u, decay.T), reverse=reverse)[1]


def exchange(uf, ub, totals):
    count = lax.axis_size(ALL)
    heads = totals.shape[1]
    each = uf.shape[0] // count
    everyone = lax.all_gather(totals, ALL)
    mine = lax.axis_index(ALL) * each + jnp.arange(each)
    pick = (mine[:, None] // HEAD_DIM == jnp.arange(heads)[None]).astype(f32)
    decay = jnp.exp(jnp.einsum("rh,pdh->drp", pick, everyone, precision=HIGH))
    uf, ub = (
        lax.all_to_all(u, ALL, split_axis=0, concat_axis=0, tiled=True).reshape(
            count, each, STATE
        )
        for u in (uf, ub)
    )
    if count <= 64:
        shape = jax.ShapeDtypeStruct(uf.shape, bf16)
        sf, sb = pl.pallas_call(scan_kernel, out_shape=(shape, shape))(uf, ub, decay)
    else:
        sf, sb = scan_plain(uf, decay[0], False), scan_plain(ub, decay[1], True)
    return tuple(
        lax.all_to_all(
            s.reshape(count * each, STATE), ALL, split_axis=0, concat_axis=0, tiled=True
        )
        for s in (sf, sb)
    )


def local(x, b, c, gate, ahead, back, fade, x_taps, b_taps, c_taps, offsets, exponents, gain):
    tokens, x_width = x.shape[1:]
    b_width = b.shape[2]
    heads = ahead.shape[2]
    steps = heads // STEP_HEADS
    xs, bs = x_width // steps, b_width // steps
    wide, deep = lax.axis_size("sp"), lax.axis_size("dp")
    order = [s * deep + d for d in range(deep) for s in range(wide)]
    up = list(zip(order[:-1], order[1:]))
    down = [(target, source) for source, target in up]

    def edge(rows):
        return jnp.concatenate([x[0, rows], b[0, rows], c[0, rows]], axis=1)

    low = lax.ppermute(edge(slice(tokens - 2, tokens)), ("sp", "dp"), up)
    high = lax.ppermute(edge(slice(0, 1)), ("sp", "dp"), down)
    width = low.shape[1]
    halo = jnp.concatenate(
        [jnp.zeros((6, width), bf16), low, high, jnp.zeros((7, width), bf16)], axis=0
    )
    mine = [t.astype(f32) for t in (x_taps, b_taps, c_taps)]
    mine.append(jnp.concatenate([offsets, exponents], axis=0))
    bounds = [0]
    for piece in mine:
        bounds.append(bounds[-1] + piece.shape[1])
    gathered = lax.all_gather(jnp.concatenate(mine, axis=1), "sp")
    xt, bt, ct, params = (
        jnp.transpose(gathered[:, :, lo:hi], (1, 0, 2)).reshape(gathered.shape[1], -1)
        for lo, hi in zip(bounds[:-1], bounds[1:])
    )
    cols, rows, totals = pl.pallas_call(
        rates_kernel,
        out_shape=(
            jax.ShapeDtypeStruct((steps, BLK, 128), f32),
            jax.ShapeDtypeStruct((steps, 4 * SLOT, BLK), f32),
            jax.ShapeDtypeStruct((2, heads), f32),
        ),
    )(ahead, back, fade, params)

    def raw(size):
        return pl.BlockSpec((1, tokens, size), lambda g: (0, 0, g))

    def flat(rows_, size, start=0):
        return pl.BlockSpec((rows_, size), lambda g: (0, start + g))

    def stacked(rows_, size=128):
        return pl.BlockSpec((1, rows_, size), lambda g: (g, 0, 0))

    state_spec = pl.BlockSpec((xs, STATE), lambda g: (g, 0))
    taps = xt.shape[0]
    params_ = pltpu.CompilerParams(dimension_semantics=("arbitrary",))
    xc, bc, cc, uf, ub = pl.pallas_call(
        state_kernel,
        grid=(steps,),
        in_specs=[
            raw(xs),
            raw(bs),
            raw(bs),
            flat(16, xs),
            flat(16, bs, x_width // bs),
            flat(16, bs, (x_width + b_width) // bs),
            flat(taps, xs),
            flat(taps, bs),
            flat(taps, bs),
            stacked(BLK),
        ],
        out_specs=[flat(tokens, xs), flat(tokens, bs), flat(tokens, bs), state_spec, state_spec],
        out_shape=[
            jax.ShapeDtypeStruct((tokens, x_width), bf16),
            jax.ShapeDtypeStruct((tokens, b_width), bf16),
            jax.ShapeDtypeStruct((tokens, b_width), bf16),
            jax.ShapeDtypeStruct((x_width, STATE), bf16),
            jax.ShapeDtypeStruct((x_width, STATE), bf16),
        ],
        compiler_params=params_,
    )(x, b, c, halo, halo, halo, xt, bt, ct, cols)
    y = pl.pallas_call(
        block_kernel,
        grid=(steps,),
        in_specs=[
            flat(tokens, xs),
            flat(tokens, bs),
            flat(tokens, bs),
            stacked(BLK),
            stacked(4 * SLOT),
        ],
        out_specs=flat(tokens, xs),
        out_shape=jax.ShapeDtypeStruct((tokens, x_width), f32),
        compiler_params=params_,
    )(xc, bc, cc, cols, rows)
    sf, sb = exchange(uf, ub, totals)
    return pl.pallas_call(
        finish_kernel,
        grid=(steps,),
        in_specs=[
            flat(tokens, xs),
            flat(tokens, bs),
            stacked(BLK),
            state_spec,
            state_spec,
            raw(xs),
            flat(1, xs),
        ],
        out_specs=raw(xs),
        out_shape=jax.ShapeDtypeStruct(x.shape, bf16),
        compiler_params=params_,
    )(y, cc, cols, sf, sb, gate, gain[None])


def solution(mesh):
    token = P("dp", "sp", None)
    placed = (token,) * 7 + (P(None, "sp"),) * 5 + (P(),)
    return jax.shard_map(local, mesh=mesh, in_specs=placed, out_specs=token, check_vma=False)
```

```python
import jax
import jax.numpy as jnp
from jax import lax
from jax.experimental import pallas as pl
from jax.experimental.pallas import tpu as pltpu
from jax.sharding import PartitionSpec as P

HEAD_DIM = 64
STATE = 128
BLK = 128
HIGH = lax.Precision.HIGHEST
f32 = jnp.float32
bf16 = jnp.bfloat16
ALL = ("dp", "sp")
STEP_HEADS = 6
SLOT = 8
RF, RB, CF, CB, FF, FB, EF, EB = range(8)


def iota(shape, dim):
    return lax.broadcasted_iota(jnp.int32, shape, dim)


def rates_kernel(ahead, back, fade, params, cols, rows, totals):
    steps = cols.shape[0]
    spread = fade[0]
    tri = iota((BLK, BLK), 0) - iota((BLK, BLK), 1)

    def one(raw, d, mask):
        rate = jax.nn.softplus(raw + params[d : d + 1, :])
        log = -jnp.exp(params[2 + d : 3 + d, :]) * rate + spread
        cum = jnp.dot(mask.astype(f32), log, precision=HIGH, preferred_element_type=f32)
        return rate, cum

    rate_f, cum_f = one(ahead[0], 0, tri >= 0)
    rate_b, cum_b = one(back[0], 1, tri <= 0)
    tot_f, tot_b = cum_f[BLK - 1 :], cum_b[:1]
    parts = (
        rate_f,
        rate_b,
        cum_f,
        cum_b,
        rate_f * jnp.exp(tot_f - cum_f),
        rate_b * jnp.exp(tot_b - cum_b),
        jnp.exp(cum_f),
        jnp.exp(cum_b),
    )
    gap = jnp.zeros((BLK, SLOT - STEP_HEADS), f32)
    rest = jnp.zeros((BLK, 128 - SLOT * len(parts)), f32)
    for g in range(steps):
        at = slice(g * STEP_HEADS, (g + 1) * STEP_HEADS)
        pieces = []
        for part in parts:
            pieces += [part[:, at], gap]
        packed = jnp.concatenate(pieces + [rest], axis=1)
        cols[g] = packed
        turned = packed.T[: 4 * SLOT]
        rows[g] = turned
        for d, (start, end) in enumerate(((CF * SLOT, BLK - 1), (CB * SLOT, 0))):
            last = turned[start : start + STEP_HEADS, end : end + 1]
            totals[d, at] = jnp.broadcast_to(last, (STEP_HEADS, 128))


def expand(cols, which, width):
    pick = iota((128, width), 0) == which * SLOT + iota((128, width), 1) // HEAD_DIM
    return jnp.dot(cols, pick.astype(f32), precision=HIGH, preferred_element_type=f32)


def conv(ref, halo, taps):
    edge = halo[...].astype(f32)
    full = jnp.concatenate([edge[:8], ref[0].astype(f32), edge[8:]], axis=0)
    total = full[6 : 6 + BLK] * taps[0:1]
    for k in range(1, taps.shape[0]):
        total = total + full[6 + k : 6 + k + BLK] * taps[k : k + 1]
    return jax.nn.silu(total).astype(bf16)


def state_kernel(place, x, b, c, xh, bh, ch, xt, bt, ct, cols, xo, bo, co, send, keep):
    xc, bc = conv(x, xh, xt), conv(b, bh, bt)
    xo[...] = xc
    bo[...] = bc
    co[...] = conv(c, ch, ct)
    width = xc.shape[1]
    half = width // 2
    packed = cols[0]
    xf = xc.astype(f32)
    both = []
    for which in (FF, FB):
        scaled = (xf * expand(packed, which, width)).astype(bf16)
        full = lax.dot_general(
            scaled, bc, (((0,), (0,)), ((), ())), preferred_element_type=f32
        )
        both.append((full[:half, :STATE].astype(bf16), full[half:, STATE:].astype(bf16)))

    def put(out):
        for d in range(2):
            out[d, :half], out[d, half:] = both[d]

    turn = pl.program_id(0)
    pl.when(turn < pl.num_programs(0) // 2)(lambda: put(send))
    pl.when(turn >= pl.num_programs(0) // 2)(lambda: put(keep))


def block_kernel(x, b, c, cols, rows, out):
    packed, across = cols[0], rows[0]
    ahead = iota((BLK, BLK), 1) - iota((BLK, BLK), 0)
    lower, upper = ahead < 0, ahead > 0
    lane = iota((BLK, 128), 1)
    scores = [
        lax.dot_general(
            c[:, i * STATE : (i + 1) * STATE],
            b[:, i * STATE : (i + 1) * STATE],
            (((1,), (1,)), ((), ())),
            preferred_element_type=f32,
        )
        for i in range(2)
    ]

    def head(j, pair):
        def col(a):
            return packed[:, a * SLOT + j : a * SLOT + j + 1]

        def row(a):
            return across[a * SLOT + j : a * SLOT + j + 1]

        gaps = jnp.where(lower, col(CF) - row(CF), col(CB) - row(CB))
        rate = jnp.where(lower, row(RF), jnp.where(upper, row(RB), row(RF) + row(RB)))
        weights = (scores[j * 2 // STEP_HEADS] * jnp.exp(gaps) * rate).astype(bf16)
        return jnp.dot(weights, pair, preferred_element_type=f32)

    for k in range(STEP_HEADS // 2):
        at = slice(k * 128, (k + 1) * 128)
        pair = x[:, at]
        out[:, at] = jnp.where(lane < HEAD_DIM, head(2 * k, pair), head(2 * k + 1, pair))


def finish_kernel(place, local, c, cols, mine, theirs, gate, gain, out):
    own = pl.program_id(0) < pl.num_programs(0) // 2
    packed = cols[0]
    width = local.shape[1]
    first = iota((BLK, width), 1) < width // 2
    y = local[...]
    for d, which in enumerate((EF, EB)):
        state = jnp.where(own, mine[d], theirs[d])
        by_group = [
            lax.dot_general(
                c[:, i * STATE : (i + 1) * STATE],
                state,
                (((1,), (1,)), ((), ())),
                preferred_element_type=f32,
            )
            for i in range(2)
        ]
        y = y + jnp.where(first, by_group[0], by_group[1]) * expand(packed, which, width)
    gated = y.astype(bf16).astype(f32) * jax.nn.silu(gate[0].astype(f32))
    same = iota((width, width), 0) // HEAD_DIM == iota((width, width), 1) // HEAD_DIM
    mean = jnp.dot(
        gated * gated,
        jnp.where(same, 1.0 / HEAD_DIM, 0.0),
        precision=HIGH,
        preferred_element_type=f32,
    )
    out[0] = (gated * lax.rsqrt(mean + 1e-6) * gain[...].astype(f32)).astype(bf16)


def scan_kernel(uf, ub, decay, of, ob):
    count = uf.shape[0]
    state = jnp.zeros(uf.shape[1:], f32)
    for p in range(count):
        of[p] = state.astype(bf16)
        state = state * decay[0][:, p : p + 1] + uf[p].astype(f32)
    state = jnp.zeros(uf.shape[1:], f32)
    for p in reversed(range(count)):
        ob[p] = state.astype(bf16)
        state = state * decay[1][:, p : p + 1] + ub[p].astype(f32)


def scan_plain(u, decay, reverse):
    def step(state, piece):
        update, factor = piece
        return state * factor[:, None] + update.astype(f32), state.astype(bf16)

    return lax.scan(step, jnp.zeros(u.shape[1:], f32), (u, decay.T), reverse=reverse)[1]


def exchange(uf, ub, totals):
    count = lax.axis_size(ALL)
    heads = totals.shape[1]
    each = uf.shape[0] // count
    everyone = lax.all_gather(totals, ALL)
    mine = lax.axis_index(ALL) * each + jnp.arange(each)
    pick = (mine[:, None] // HEAD_DIM == jnp.arange(heads)[None]).astype(f32)
    decay = jnp.exp(jnp.einsum("rh,pdh->drp", pick, everyone, precision=HIGH))
    uf, ub = (
        lax.all_to_all(u, ALL, split_axis=0, concat_axis=0, tiled=True).reshape(
            count, each, STATE
        )
        for u in (uf, ub)
    )
    if count <= 64:
        shape = jax.ShapeDtypeStruct(uf.shape, bf16)
        sf, sb = pl.pallas_call(scan_kernel, out_shape=(shape, shape))(uf, ub, decay)
    else:
        sf, sb = scan_plain(uf, decay[0], False), scan_plain(ub, decay[1], True)
    return tuple(
        lax.all_to_all(
            s.reshape(count * each, STATE), ALL, split_axis=0, concat_axis=0, tiled=True
        )
        for s in (sf, sb)
    )


def pair_kernel(place, mine, theirs, own, par, send, keep):
    early, fwd = place[0] == 0, place[1] == 1
    e_own, e_par = jnp.exp(own[...]), jnp.exp(par[...])
    scale_mine = (jnp.where(early, e_par[0], 1.0), jnp.where(early, 1.0, e_par[1]))
    scale_theirs = (jnp.where(early, 1.0, e_own[0]), jnp.where(early, e_own[1], 1.0))
    for h in range(own.shape[1]):
        at = slice(h * HEAD_DIM, (h + 1) * HEAD_DIM)
        f, b = (
            mine[d, at].astype(f32) * scale_mine[d][h : h + 1]
            + theirs[d, at].astype(f32) * scale_theirs[d][h : h + 1]
            for d in range(2)
        )
        keep[at] = jnp.where(fwd, f, b).astype(bf16)
        send[at] = jnp.where(fwd, b, f).astype(bf16)


def segment_kernel(place, keep, got, pair, xpair, out):
    fwd = place[1] == 1
    here = jnp.where(fwd, pair[0], pair[1])
    there = jnp.where(fwd, xpair[0], xpair[1])
    factor, total = jnp.exp(here), jnp.exp(here + there)
    high = total.astype(bf16)
    middle = (total - high.astype(f32)).astype(bf16)
    lowest = (total - high.astype(f32) - middle.astype(f32)).astype(bf16)
    parts = [part.astype(f32) for part in (high, middle, lowest)]
    chunks = out.shape[0]
    each = pair.shape[1] // chunks
    rows = each * HEAD_DIM
    for j in range(chunks):
        lines = []
        for i in range(each):
            h = j * each + i
            at = slice(h * HEAD_DIM, (h + 1) * HEAD_DIM)
            new = keep[at].astype(f32) + got[at].astype(f32) * factor[h : h + 1]
            out[j, i * HEAD_DIM : (i + 1) * HEAD_DIM] = new.astype(bf16)
            lines += [part[h : h + 1] for part in parts]
        lines.append(jnp.zeros((out.shape[1] - rows - len(lines), STATE), f32))
        out[j, rows:] = jnp.concatenate(lines, axis=0).astype(bf16)


def carry_kernel(place, v, out):
    fwd = place[1] == 1
    count, rows = out.shape[:2]
    each = rows // HEAD_DIM
    state = [jnp.zeros((HEAD_DIM, STATE), f32)] * each
    for i in range(count):
        q = jnp.where(fwd, i, count - 1 - i)
        piece = v[q].astype(f32)
        lines = piece[rows:]
        for h in range(each):
            at = slice(h * HEAD_DIM, (h + 1) * HEAD_DIM)
            out[q, at] = state[h].astype(bf16)
            factor = lines[3 * h : 3 * h + 1] + lines[3 * h + 1 : 3 * h + 2]
            factor = factor + lines[3 * h + 2 : 3 * h + 3]
            state[h] = state[h] * factor + piece[at]


def enter_kernel(place, entry, other, got, mine, theirs, own, par, xpair, keep, send):
    early, fwd = place[0] == 0, place[1] == 1
    e_own, e_par = jnp.exp(own[...]), jnp.exp(par[...])
    past = jnp.exp(jnp.where(fwd, xpair[0], xpair[1]))
    for h in range(own.shape[1]):
        at = slice(h * HEAD_DIM, (h + 1) * HEAD_DIM)
        line = slice(h, h + 1)
        near = entry[at].astype(f32) * past[line] + got[at].astype(f32)
        far = other[at].astype(f32)
        f, b = jnp.where(fwd, near, far), jnp.where(fwd, far, near)
        f_mine = f * e_par[0, line] + theirs[0, at].astype(f32)
        b_mine = b * e_par[1, line] + theirs[1, at].astype(f32)
        f_theirs = f * e_own[0, line] + mine[0, at].astype(f32)
        b_theirs = b * e_own[1, line] + mine[1, at].astype(f32)
        keep[0, at] = jnp.where(early, f, f_mine).astype(bf16)
        keep[1, at] = jnp.where(early, b_mine, b).astype(bf16)
        send[0, at] = jnp.where(early, f_theirs, f).astype(bf16)
        send[1, at] = jnp.where(early, b, b_theirs).astype(bf16)


def swap(a, bit):
    wide, deep = lax.axis_size("sp"), lax.axis_size("dp")
    perm = [
        (s * deep + d, (s ^ bit) * deep + d) for s in range(wide) for d in range(deep)
    ]
    return lax.ppermute(a, ("sp", "dp"), perm)


def run(kernel, shapes, place, *args):
    smem = pl.BlockSpec(memory_space=pltpu.SMEM)
    vmem = pl.BlockSpec(memory_space=pltpu.VMEM)
    return pl.pallas_call(
        kernel,
        in_specs=[smem] + [vmem] * len(args),
        out_shape=[jax.ShapeDtypeStruct(shape, bf16) for shape in shapes],
    )(place, *args)


def exchange_tree(send, keep, logs, place):
    deep = lax.axis_size("dp")
    half = logs.shape[1] // 2
    whole_par = swap(logs, 1)
    whole_pair = logs + whole_par
    whole_xpair = swap(whole_pair, 2)
    own, par, pair, xpair = (
        lax.dynamic_slice_in_dim(a, place[0] * half, half, axis=1)
        for a in (logs, whole_par, whole_pair, whole_xpair)
    )
    theirs = swap(send, 1)
    rows = keep.shape[1:]
    across, stay = run(pair_kernel, (rows, rows), place, keep, theirs, own, par)
    got = swap(across, 2)
    each = rows[0] // deep
    (packed,) = run(segment_kernel, ((deep, each + 16, STATE),), place, stay, got, pair, xpair)
    packed = lax.all_to_all(packed, "dp", split_axis=0, concat_axis=0)
    (entry,) = run(carry_kernel, ((deep, each, STATE),), place, packed)
    entry = lax.all_to_all(entry, "dp", split_axis=0, concat_axis=0).reshape(rows)
    other = swap(entry, 2)
    mine, back = run(
        enter_kernel, (keep.shape,) * 2, place, entry, other, got, keep, theirs, own, par, xpair
    )
    return mine, swap(back, 1)


def local(x, b, c, gate, ahead, back, fade, x_taps, b_taps, c_taps, offsets, exponents, gain):
    tokens, x_width = x.shape[1:]
    b_width = b.shape[2]
    heads = ahead.shape[2]
    steps = heads // STEP_HEADS
    xs, bs = x_width // steps, b_width // steps
    wide, deep = lax.axis_size("sp"), lax.axis_size("dp")
    order = [s * deep + d for d in range(deep) for s in range(wide)]
    up = list(zip(order[:-1], order[1:]))
    down = [(target, source) for source, target in up]

    def edge(rows):
        return jnp.concatenate([x[0, rows], b[0, rows], c[0, rows]], axis=1)

    low = lax.ppermute(edge(slice(tokens - 2, tokens)), ("sp", "dp"), up)
    high = lax.ppermute(edge(slice(0, 1)), ("sp", "dp"), down)
    width = low.shape[1]
    halo = jnp.concatenate(
        [jnp.zeros((6, width), bf16), low, high, jnp.zeros((7, width), bf16)], axis=0
    )
    mine = [t.astype(f32) for t in (x_taps, b_taps, c_taps)]
    mine.append(jnp.concatenate([offsets, exponents], axis=0))
    bounds = [0]
    for piece in mine:
        bounds.append(bounds[-1] + piece.shape[1])
    gathered = lax.all_gather(jnp.concatenate(mine, axis=1), "sp")
    xt, bt, ct, params = (
        jnp.transpose(gathered[:, :, lo:hi], (1, 0, 2)).reshape(gathered.shape[1], -1)
        for lo, hi in zip(bounds[:-1], bounds[1:])
    )
    cols, rows, totals = pl.pallas_call(
        rates_kernel,
        out_shape=(
            jax.ShapeDtypeStruct((steps, BLK, 128), f32),
            jax.ShapeDtypeStruct((steps, 4 * SLOT, BLK), f32),
            jax.ShapeDtypeStruct((2, heads, 128), f32),
        ),
    )(ahead, back, fade, params)

    def raw(size):
        return pl.BlockSpec((1, tokens, size), lambda g: (0, 0, g))

    def flat(rows_, size, start=0):
        return pl.BlockSpec((rows_, size), lambda g: (0, start + g))

    def stacked(rows_, size=128):
        return pl.BlockSpec((1, rows_, size), lambda g: (g, 0, 0))

    taps = xt.shape[0]
    params_ = pltpu.CompilerParams(dimension_semantics=("arbitrary",))
    tree = wide == 4 and heads % (2 * deep) == 0 and 3 * heads // (2 * deep) <= 16
    if tree:
        spot = lax.axis_index("sp")
        place = jnp.stack([spot % 2, spot // 2]).astype(jnp.int32)
    else:
        place = jnp.zeros((2,), jnp.int32)
    middle = steps // 2

    def shifted(spec, late):
        index = spec.index_map

        def move(g, place):
            return index((g + middle * jnp.where(late, 1 - place[0], place[0])) % steps)

        return pl.BlockSpec(spec.block_shape, move)

    def sided(first):
        def move(g, place):
            return (0, jnp.minimum(g, middle - 1) if first else jnp.maximum(g - middle, 0), 0)

        return pl.BlockSpec((2, xs, STATE), move)

    def half_call(kernel, ins, in_sides, outs, out_sides, late, shapes):
        return pl.pallas_call(
            kernel,
            grid_spec=pltpu.PrefetchScalarGridSpec(
                num_scalar_prefetch=1,
                grid=(steps,),
                in_specs=[shifted(spec, late) for spec in ins[:in_sides[0]]]
                + [sided(first) for first in in_sides[1]]
                + [shifted(spec, late) for spec in ins[in_sides[0] :]],
                out_specs=[shifted(spec, late) for spec in outs] + [sided(f) for f in out_sides],
            ),
            out_shape=shapes,
            compiler_params=params_,
        )
    xc, bc, cc, send, keep = half_call(
        state_kernel,
        [
            raw(xs),
            raw(bs),
            raw(bs),
            flat(16, xs),
            flat(16, bs, x_width // bs),
            flat(16, bs, (x_width + b_width) // bs),
            flat(taps, xs),
            flat(taps, bs),
            flat(taps, bs),
            stacked(BLK),
        ],
        (10, ()),
        [flat(tokens, xs), flat(tokens, bs), flat(tokens, bs)],
        (True, False),
        True,
        [
            jax.ShapeDtypeStruct((tokens, x_width), bf16),
            jax.ShapeDtypeStruct((tokens, b_width), bf16),
            jax.ShapeDtypeStruct((tokens, b_width), bf16),
            jax.ShapeDtypeStruct((2, x_width // 2, STATE), bf16),
            jax.ShapeDtypeStruct((2, x_width // 2, STATE), bf16),
        ],
    )(place, x, b, c, halo, halo, halo, xt, bt, ct, cols)
    y = pl.pallas_call(
        block_kernel,
        grid=(steps,),
        in_specs=[
            flat(tokens, xs),
            flat(tokens, bs),
            flat(tokens, bs),
            stacked(BLK),
            stacked(4 * SLOT),
        ],
        out_specs=flat(tokens, xs),
        out_shape=jax.ShapeDtypeStruct((tokens, x_width), f32),
        compiler_params=params_,
    )(xc, bc, cc, cols, rows)
    if tree:
        mine, theirs = exchange_tree(send, keep, totals, place)
    else:
        uf, ub = (jnp.concatenate([keep[d], send[d]], axis=0) for d in range(2))
        states = jnp.stack(exchange(uf, ub, totals[:, :, 0]))
        mine, theirs = states[:, : x_width // 2], states[:, x_width // 2 :]
    (out,) = half_call(
        finish_kernel,
        [flat(tokens, xs), flat(tokens, bs), stacked(BLK), raw(xs), flat(1, xs)],
        (3, (True, False)),
        [raw(xs)],
        (),
        False,
        [jax.ShapeDtypeStruct(x.shape, bf16)],
    )(place, y, cc, cols, mine, theirs, gate, gain[None])
    return out


def solution(mesh):
    token = P("dp", "sp", None)
    placed = (token,) * 7 + (P(None, "sp"),) * 5 + (P(),)
    return jax.shard_map(local, mesh=mesh, in_specs=placed, out_specs=token, check_vma=False)
```

```python
import jax
import jax.numpy as jnp
from jax import lax
from jax.experimental import pallas as pl
from jax.experimental.pallas import tpu as pltpu
from jax.sharding import PartitionSpec as P

HEAD_DIM = 64
STATE = 128
BLK = 128
HIGH = lax.Precision.HIGHEST
f32 = jnp.float32
bf16 = jnp.bfloat16
ALL = ("dp", "sp")
STEP_HEADS = 6
SLOT = 8
RF, RB, CF, CB, FF, FB, EF, EB = range(8)


def iota(shape, dim):
    return lax.broadcasted_iota(jnp.int32, shape, dim)


def rates_kernel(ahead, back, fade, params, cols, rows, totals):
    steps = cols.shape[0]
    spread = fade[0]
    tri = iota((BLK, BLK), 0) - iota((BLK, BLK), 1)

    def one(raw, d, mask):
        rate = jax.nn.softplus(raw + params[:, d : d + 1])
        log = -jnp.exp(params[:, 2 + d : 3 + d]) * rate + spread
        cum = jnp.dot(log, mask.astype(f32), precision=HIGH, preferred_element_type=f32)
        return rate, cum

    rate_f, cum_f = one(ahead[0], 0, tri <= 0)
    rate_b, cum_b = one(back[0], 1, tri >= 0)
    tot_f, tot_b = cum_f[:, BLK - 1 :], cum_b[:, :1]
    totals[0] = jnp.broadcast_to(tot_f, totals.shape[1:])
    totals[1] = jnp.broadcast_to(tot_b, totals.shape[1:])
    parts = (
        rate_f,
        rate_b,
        cum_f,
        cum_b,
        rate_f * jnp.exp(tot_f - cum_f),
        rate_b * jnp.exp(tot_b - cum_b),
        jnp.exp(cum_f),
        jnp.exp(cum_b),
    )
    gap = jnp.zeros((SLOT - STEP_HEADS, BLK), f32)
    rest = jnp.zeros((128 - SLOT * len(parts), BLK), f32)
    for g in range(steps):
        at = slice(g * STEP_HEADS, (g + 1) * STEP_HEADS)
        pieces = []
        for part in parts:
            pieces += [part[at], gap]
        packed = jnp.concatenate(pieces + [rest], axis=0)
        rows[g] = packed[: 4 * SLOT]
        cols[g] = packed.T


def expand(cols, which, width):
    first = iota((BLK, 128), 1) < HEAD_DIM
    start = which * SLOT
    return jnp.concatenate(
        [
            jnp.where(first, cols[:, j : j + 1], cols[:, j + 1 : j + 2])
            for j in range(start, start + width // HEAD_DIM, 2)
        ],
        axis=1,
    )


def conv(ref, halo, taps):
    edge = halo[...].astype(f32)
    full = jnp.concatenate([edge[:8], ref[0].astype(f32), edge[8:]], axis=0)
    total = full[6 : 6 + BLK] * taps[0:1]
    for k in range(1, taps.shape[0]):
        total = total + full[6 + k : 6 + k + BLK] * taps[k : k + 1]
    return jax.nn.silu(total).astype(bf16)


def state_kernel(place, x, b, c, xh, bh, ch, xt, bt, ct, cols, xo, bo, co, send, keep):
    xc, bc = conv(x, xh, xt), conv(b, bh, bt)
    xo[...] = xc
    bo[...] = bc
    co[...] = conv(c, ch, ct)
    width = xc.shape[1]
    half = width // 2
    packed = cols[0]
    xf = xc.astype(f32)
    both = []
    for which in (FF, FB):
        scaled = (xf * expand(packed, which, width)).astype(bf16)
        full = lax.dot_general(
            scaled, bc, (((0,), (0,)), ((), ())), preferred_element_type=f32
        )
        both.append((full[:half, :STATE].astype(bf16), full[half:, STATE:].astype(bf16)))

    def put(out):
        for d in range(2):
            out[d, :half], out[d, half:] = both[d]

    turn = pl.program_id(0)
    pl.when(turn < pl.num_programs(0) // 2)(lambda: put(send))
    pl.when(turn >= pl.num_programs(0) // 2)(lambda: put(keep))


def block_kernel(x, b, c, cols, rows, out):
    packed, across = cols[0], rows[0]
    ahead = iota((BLK, BLK), 1) - iota((BLK, BLK), 0)
    lower, upper = ahead < 0, ahead > 0
    lane = iota((BLK, 128), 1)
    scores = [
        lax.dot_general(
            c[:, i * STATE : (i + 1) * STATE],
            b[:, i * STATE : (i + 1) * STATE],
            (((1,), (1,)), ((), ())),
            preferred_element_type=f32,
        )
        for i in range(2)
    ]

    def head(j, pair):
        def col(a):
            return packed[:, a * SLOT + j : a * SLOT + j + 1]

        def row(a):
            return across[a * SLOT + j : a * SLOT + j + 1]

        gaps = jnp.where(lower, col(CF) - row(CF), col(CB) - row(CB))
        rate = jnp.where(lower, row(RF), jnp.where(upper, row(RB), row(RF) + row(RB)))
        weights = (scores[j * 2 // STEP_HEADS] * jnp.exp(gaps) * rate).astype(bf16)
        return jnp.dot(weights, pair, preferred_element_type=f32)

    for k in range(STEP_HEADS // 2):
        at = slice(k * 128, (k + 1) * 128)
        pair = x[:, at]
        out[:, at] = jnp.where(lane < HEAD_DIM, head(2 * k, pair), head(2 * k + 1, pair))


def finish_kernel(place, local, c, cols, mine, theirs, gate, gain, out):
    own = pl.program_id(0) < pl.num_programs(0) // 2
    packed = cols[0]
    width = local.shape[1]
    first = iota((BLK, width), 1) < width // 2
    y = local[...]
    for d, which in enumerate((EF, EB)):
        state = jnp.where(own, mine[d], theirs[d])
        by_group = [
            lax.dot_general(
                c[:, i * STATE : (i + 1) * STATE],
                state,
                (((1,), (1,)), ((), ())),
                preferred_element_type=f32,
            )
            for i in range(2)
        ]
        y = y + jnp.where(first, by_group[0], by_group[1]) * expand(packed, which, width)
    gated = y.astype(bf16).astype(f32) * jax.nn.silu(gate[0].astype(f32))
    same = iota((128, 128), 0) // HEAD_DIM == iota((128, 128), 1) // HEAD_DIM
    ones = jnp.where(same, 1.0 / HEAD_DIM, 0.0).astype(bf16)
    square = gated * gated
    high = square.astype(bf16)
    low = (square - high.astype(f32)).astype(bf16)
    mean = jnp.concatenate(
        [
            jnp.dot(high[:, k : k + 128], ones, preferred_element_type=f32)
            + jnp.dot(low[:, k : k + 128], ones, preferred_element_type=f32)
            for k in range(0, width, 128)
        ],
        axis=1,
    )
    out[0] = (gated * lax.rsqrt(mean + 1e-6) * gain[...].astype(f32)).astype(bf16)


def scan_kernel(uf, ub, decay, of, ob):
    count = uf.shape[0]
    state = jnp.zeros(uf.shape[1:], f32)
    for p in range(count):
        of[p] = state.astype(bf16)
        state = state * decay[0][:, p : p + 1] + uf[p].astype(f32)
    state = jnp.zeros(uf.shape[1:], f32)
    for p in reversed(range(count)):
        ob[p] = state.astype(bf16)
        state = state * decay[1][:, p : p + 1] + ub[p].astype(f32)


def scan_plain(u, decay, reverse):
    def step(state, piece):
        update, factor = piece
        return state * factor[:, None] + update.astype(f32), state.astype(bf16)

    return lax.scan(step, jnp.zeros(u.shape[1:], f32), (u, decay.T), reverse=reverse)[1]


def exchange(uf, ub, totals):
    count = lax.axis_size(ALL)
    heads = totals.shape[1]
    each = uf.shape[0] // count
    everyone = lax.all_gather(totals, ALL)
    mine = lax.axis_index(ALL) * each + jnp.arange(each)
    pick = (mine[:, None] // HEAD_DIM == jnp.arange(heads)[None]).astype(f32)
    decay = jnp.exp(jnp.einsum("rh,pdh->drp", pick, everyone, precision=HIGH))
    uf, ub = (
        lax.all_to_all(u, ALL, split_axis=0, concat_axis=0, tiled=True).reshape(
            count, each, STATE
        )
        for u in (uf, ub)
    )
    if count <= 64:
        shape = jax.ShapeDtypeStruct(uf.shape, bf16)
        sf, sb = pl.pallas_call(scan_kernel, out_shape=(shape, shape))(uf, ub, decay)
    else:
        sf, sb = scan_plain(uf, decay[0], False), scan_plain(ub, decay[1], True)
    return tuple(
        lax.all_to_all(
            s.reshape(count * each, STATE), ALL, split_axis=0, concat_axis=0, tiled=True
        )
        for s in (sf, sb)
    )


def pair_kernel(place, mine, theirs, own, par, send, keep):
    early, fwd = place[0] == 0, place[1] == 1
    e_own, e_par = jnp.exp(own[...]), jnp.exp(par[...])
    scale_mine = (jnp.where(early, e_par[0], 1.0), jnp.where(early, 1.0, e_par[1]))
    scale_theirs = (jnp.where(early, 1.0, e_own[0]), jnp.where(early, e_own[1], 1.0))
    for h in range(own.shape[1]):
        at = slice(h * HEAD_DIM, (h + 1) * HEAD_DIM)
        f, b = (
            mine[d, at].astype(f32) * scale_mine[d][h : h + 1]
            + theirs[d, at].astype(f32) * scale_theirs[d][h : h + 1]
            for d in range(2)
        )
        keep[at] = jnp.where(fwd, f, b).astype(bf16)
        send[at] = jnp.where(fwd, b, f).astype(bf16)


def segment_kernel(place, keep, got, pair, xpair, out):
    fwd = place[1] == 1
    here = jnp.where(fwd, pair[0], pair[1])
    there = jnp.where(fwd, xpair[0], xpair[1])
    factor, total = jnp.exp(here), jnp.exp(here + there)
    high = total.astype(bf16)
    middle = (total - high.astype(f32)).astype(bf16)
    lowest = (total - high.astype(f32) - middle.astype(f32)).astype(bf16)
    parts = [part.astype(f32) for part in (high, middle, lowest)]
    chunks = out.shape[0]
    each = pair.shape[1] // chunks
    rows = each * HEAD_DIM
    for j in range(chunks):
        lines = []
        for i in range(each):
            h = j * each + i
            at = slice(h * HEAD_DIM, (h + 1) * HEAD_DIM)
            new = keep[at].astype(f32) + got[at].astype(f32) * factor[h : h + 1]
            out[j, i * HEAD_DIM : (i + 1) * HEAD_DIM] = new.astype(bf16)
            lines += [part[h : h + 1] for part in parts]
        lines.append(jnp.zeros((out.shape[1] - rows - len(lines), STATE), f32))
        out[j, rows:] = jnp.concatenate(lines, axis=0).astype(bf16)


def carry_kernel(place, v, out):
    fwd = place[1] == 1
    count, rows = out.shape[:2]
    each = rows // HEAD_DIM
    state = [jnp.zeros((HEAD_DIM, STATE), f32)] * each
    for i in range(count):
        q = jnp.where(fwd, i, count - 1 - i)
        piece = v[q].astype(f32)
        lines = piece[rows:]
        for h in range(each):
            at = slice(h * HEAD_DIM, (h + 1) * HEAD_DIM)
            out[q, at] = state[h].astype(bf16)
            factor = lines[3 * h : 3 * h + 1] + lines[3 * h + 1 : 3 * h + 2]
            factor = factor + lines[3 * h + 2 : 3 * h + 3]
            state[h] = state[h] * factor + piece[at]


def enter_kernel(place, entry, other, got, mine, theirs, own, par, xpair, keep, send):
    early, fwd = place[0] == 0, place[1] == 1
    e_own, e_par = jnp.exp(own[...]), jnp.exp(par[...])
    past = jnp.exp(jnp.where(fwd, xpair[0], xpair[1]))
    for h in range(own.shape[1]):
        at = slice(h * HEAD_DIM, (h + 1) * HEAD_DIM)
        line = slice(h, h + 1)
        near = entry[at].astype(f32) * past[line] + got[at].astype(f32)
        far = other[at].astype(f32)
        f, b = jnp.where(fwd, near, far), jnp.where(fwd, far, near)
        f_mine = f * e_par[0, line] + theirs[0, at].astype(f32)
        b_mine = b * e_par[1, line] + theirs[1, at].astype(f32)
        f_theirs = f * e_own[0, line] + mine[0, at].astype(f32)
        b_theirs = b * e_own[1, line] + mine[1, at].astype(f32)
        keep[0, at] = jnp.where(early, f, f_mine).astype(bf16)
        keep[1, at] = jnp.where(early, b_mine, b).astype(bf16)
        send[0, at] = jnp.where(early, f_theirs, f).astype(bf16)
        send[1, at] = jnp.where(early, b, b_theirs).astype(bf16)


def swap(a, bit):
    wide, deep = lax.axis_size("sp"), lax.axis_size("dp")
    perm = [
        (s * deep + d, (s ^ bit) * deep + d) for s in range(wide) for d in range(deep)
    ]
    return lax.ppermute(a, ("sp", "dp"), perm)


def run(kernel, shapes, place, *args):
    smem = pl.BlockSpec(memory_space=pltpu.SMEM)
    vmem = pl.BlockSpec(memory_space=pltpu.VMEM)
    return pl.pallas_call(
        kernel,
        in_specs=[smem] + [vmem] * len(args),
        out_shape=[jax.ShapeDtypeStruct(shape, bf16) for shape in shapes],
    )(place, *args)


def exchange_tree(send, keep, logs, place, block):
    deep = lax.axis_size("dp")
    half = logs.shape[1] // 2
    whole_par = swap(logs, 1)
    whole_pair = logs + whole_par
    whole_xpair = swap(whole_pair, 2)
    own, par, pair, xpair = (
        lax.dynamic_slice_in_dim(a, place[0] * half, half, axis=1)
        for a in (logs, whole_par, whole_pair, whole_xpair)
    )
    theirs = swap(send, 1)
    rows = keep.shape[1:]
    across, stay = run(pair_kernel, (rows, rows), place, keep, theirs, own, par)
    y, got = lax.optimization_barrier((block(), swap(across, 2)))
    each = rows[0] // deep
    (packed,) = run(segment_kernel, ((deep, each + 16, STATE),), place, stay, got, pair, xpair)
    packed = lax.all_to_all(packed, "dp", split_axis=0, concat_axis=0)
    (entry,) = run(carry_kernel, ((deep, each, STATE),), place, packed)
    entry = lax.all_to_all(entry, "dp", split_axis=0, concat_axis=0).reshape(rows)
    other = swap(entry, 2)
    mine, back = run(
        enter_kernel, (keep.shape,) * 2, place, entry, other, got, keep, theirs, own, par, xpair
    )
    return mine, swap(back, 1), y


def local(x, b, c, gate, ahead, back, fade, x_taps, b_taps, c_taps, offsets, exponents, gain):
    tokens, x_width = x.shape[1:]
    b_width = b.shape[2]
    heads = ahead.shape[2]
    steps = heads // STEP_HEADS
    xs, bs = x_width // steps, b_width // steps
    wide, deep = lax.axis_size("sp"), lax.axis_size("dp")
    order = [s * deep + d for d in range(deep) for s in range(wide)]
    up = list(zip(order[:-1], order[1:]))
    down = [(target, source) for source, target in up]

    def edge(rows):
        return jnp.concatenate([x[0, rows], b[0, rows], c[0, rows]], axis=1)

    low = lax.ppermute(edge(slice(tokens - 2, tokens)), ("sp", "dp"), up)
    high = lax.ppermute(edge(slice(0, 1)), ("sp", "dp"), down)
    width = low.shape[1]
    halo = jnp.concatenate(
        [jnp.zeros((6, width), bf16), low, high, jnp.zeros((7, width), bf16)], axis=0
    )
    mine = [t.astype(f32) for t in (x_taps, b_taps, c_taps)]
    mine.append(jnp.concatenate([offsets, exponents], axis=0))
    bounds = [0]
    for piece in mine:
        bounds.append(bounds[-1] + piece.shape[1])
    gathered = lax.all_gather(jnp.concatenate(mine, axis=1), "sp")
    xt, bt, ct = (
        jnp.transpose(gathered[:, :, lo:hi], (1, 0, 2)).reshape(gathered.shape[1], -1)
        for lo, hi in zip(bounds[:-2], bounds[1:-1])
    )
    params = jnp.transpose(gathered[:, :, bounds[-2] :], (0, 2, 1)).reshape(heads, -1)
    cols, rows, totals = pl.pallas_call(
        rates_kernel,
        out_shape=(
            jax.ShapeDtypeStruct((steps, BLK, 128), f32),
            jax.ShapeDtypeStruct((steps, 4 * SLOT, BLK), f32),
            jax.ShapeDtypeStruct((2, heads, 128), f32),
        ),
    )(*(jnp.swapaxes(a, 1, 2) for a in (ahead, back, fade)), params)

    def raw(size):
        return pl.BlockSpec((1, tokens, size), lambda g: (0, 0, g))

    def flat(rows_, size, start=0):
        return pl.BlockSpec((rows_, size), lambda g: (0, start + g))

    def stacked(rows_, size=128):
        return pl.BlockSpec((1, rows_, size), lambda g: (g, 0, 0))

    taps = xt.shape[0]
    params_ = pltpu.CompilerParams(dimension_semantics=("arbitrary",))
    tree = wide == 4 and heads % (2 * deep) == 0 and 3 * heads // (2 * deep) <= 16
    if tree:
        spot = lax.axis_index("sp")
        place = jnp.stack([spot % 2, spot // 2]).astype(jnp.int32)
    else:
        place = jnp.zeros((2,), jnp.int32)
    middle = steps // 2

    def shifted(spec, late):
        index = spec.index_map

        def move(g, place):
            return index((g + middle * jnp.where(late, 1 - place[0], place[0])) % steps)

        return pl.BlockSpec(spec.block_shape, move)

    def sided(first):
        def move(g, place):
            return (0, jnp.minimum(g, middle - 1) if first else jnp.maximum(g - middle, 0), 0)

        return pl.BlockSpec((2, xs, STATE), move)

    def half_call(kernel, ins, in_sides, outs, out_sides, late, shapes):
        return pl.pallas_call(
            kernel,
            grid_spec=pltpu.PrefetchScalarGridSpec(
                num_scalar_prefetch=1,
                grid=(steps,),
                in_specs=[shifted(spec, late) for spec in ins[:in_sides[0]]]
                + [sided(first) for first in in_sides[1]]
                + [shifted(spec, late) for spec in ins[in_sides[0] :]],
                out_specs=[shifted(spec, late) for spec in outs] + [sided(f) for f in out_sides],
            ),
            out_shape=shapes,
            compiler_params=params_,
        )
    xc, bc, cc, send, keep = half_call(
        state_kernel,
        [
            raw(xs),
            raw(bs),
            raw(bs),
            flat(16, xs),
            flat(16, bs, x_width // bs),
            flat(16, bs, (x_width + b_width) // bs),
            flat(taps, xs),
            flat(taps, bs),
            flat(taps, bs),
            stacked(BLK),
        ],
        (10, ()),
        [flat(tokens, xs), flat(tokens, bs), flat(tokens, bs)],
        (True, False),
        True,
        [
            jax.ShapeDtypeStruct((tokens, x_width), bf16),
            jax.ShapeDtypeStruct((tokens, b_width), bf16),
            jax.ShapeDtypeStruct((tokens, b_width), bf16),
            jax.ShapeDtypeStruct((2, x_width // 2, STATE), bf16),
            jax.ShapeDtypeStruct((2, x_width // 2, STATE), bf16),
        ],
    )(place, x, b, c, halo, halo, halo, xt, bt, ct, cols)
    block = lambda: pl.pallas_call(
        block_kernel,
        grid=(steps,),
        in_specs=[
            flat(tokens, xs),
            flat(tokens, bs),
            flat(tokens, bs),
            stacked(BLK),
            stacked(4 * SLOT),
        ],
        out_specs=flat(tokens, xs),
        out_shape=jax.ShapeDtypeStruct((tokens, x_width), f32),
        compiler_params=params_,
    )(xc, bc, cc, cols, rows)
    if tree:
        mine, theirs, y = exchange_tree(send, keep, totals, place, block)
    else:
        y = block()
        uf, ub = (jnp.concatenate([keep[d], send[d]], axis=0) for d in range(2))
        states = jnp.stack(exchange(uf, ub, totals[:, :, 0]))
        mine, theirs = states[:, : x_width // 2], states[:, x_width // 2 :]
    (out,) = half_call(
        finish_kernel,
        [flat(tokens, xs), flat(tokens, bs), stacked(BLK), raw(xs), flat(1, xs)],
        (3, (True, False)),
        [raw(xs)],
        (),
        False,
        [jax.ShapeDtypeStruct(x.shape, bf16)],
    )(place, y, cc, cols, mine, theirs, gate, gain[None])
    return out


def solution(mesh):
    token = P("dp", "sp", None)
    placed = (token,) * 7 + (P(None, "sp"),) * 5 + (P(),)
    return jax.shard_map(local, mesh=mesh, in_specs=placed, out_specs=token, check_vma=False)
```

```python
import jax
import jax.numpy as jnp
from jax import lax
from jax.experimental import pallas as pl
from jax.experimental.pallas import tpu as pltpu
from jax.sharding import PartitionSpec as P

HEAD_DIM = 64
STATE = 128
BLK = 128
HIGH = lax.Precision.HIGHEST
f32 = jnp.float32
bf16 = jnp.bfloat16
ALL = ("dp", "sp")
STEP_HEADS = 6
SLOT = 8
RF, RB, CF, CB, FF, FB, EF, EB = range(8)


def iota(shape, dim):
    return lax.broadcasted_iota(jnp.int32, shape, dim)


def edge_kernel(xl, bl, cl, xf, bf, cf, xt, bt, ct, offsets, exponents, low, high, packed):
    at = 0
    for end, start in ((xl, xf), (bl, bf), (cl, cf)):
        to = at + end.shape[2]
        rows = end.shape[1]
        low[:, at:to] = end[0].astype(f32)[rows - 2 :].astype(bf16)
        high[:, at:to] = start[0].astype(f32)[:1].astype(bf16)
        at = to
    at = 0
    for part in (xt, bt, ct):
        packed[:, at : at + part.shape[1]] = part[...].astype(f32)
        at += part.shape[1]
    packed[0:2, at:] = offsets[...]
    packed[2:4, at:] = exponents[...]


def rates_kernel(ahead, back, fade, params, cols, rows, totals):
    steps = cols.shape[0]
    spread = fade[0]
    tri = iota((BLK, BLK), 0) - iota((BLK, BLK), 1)

    def one(raw, d, mask):
        rate = jax.nn.softplus(raw + params[:, d : d + 1])
        log = -jnp.exp(params[:, 2 + d : 3 + d]) * rate + spread
        cum = jnp.dot(log, mask.astype(f32), precision=HIGH, preferred_element_type=f32)
        return rate, cum

    rate_f, cum_f = one(ahead[0], 0, tri <= 0)
    rate_b, cum_b = one(back[0], 1, tri >= 0)
    tot_f, tot_b = cum_f[:, BLK - 1 :], cum_b[:, :1]
    totals[0] = jnp.broadcast_to(tot_f, totals.shape[1:])
    totals[1] = jnp.broadcast_to(tot_b, totals.shape[1:])
    parts = (
        rate_f,
        rate_b,
        cum_f,
        cum_b,
        rate_f * jnp.exp(tot_f - cum_f),
        rate_b * jnp.exp(tot_b - cum_b),
        jnp.exp(cum_f),
        jnp.exp(cum_b),
    )
    gap = jnp.zeros((SLOT - STEP_HEADS, BLK), f32)
    rest = jnp.zeros((128 - SLOT * len(parts), BLK), f32)
    for g in range(steps):
        at = slice(g * STEP_HEADS, (g + 1) * STEP_HEADS)
        pieces = []
        for part in parts:
            pieces += [part[at], gap]
        packed = jnp.concatenate(pieces + [rest], axis=0)
        rows[g] = packed[: 4 * SLOT]
        cols[g] = packed.T


def expand(cols, which, width):
    first = iota((BLK, 128), 1) < HEAD_DIM
    start = which * SLOT
    return jnp.concatenate(
        [
            jnp.where(first, cols[:, j : j + 1], cols[:, j + 1 : j + 2])
            for j in range(start, start + width // HEAD_DIM, 2)
        ],
        axis=1,
    )


def conv(ref, halo, taps):
    edge = halo[...].astype(f32)
    full = jnp.concatenate([edge[:8], ref[0].astype(f32), edge[8:]], axis=0)
    total = full[6 : 6 + BLK] * taps[0:1]
    for k in range(1, taps.shape[0]):
        total = total + full[6 + k : 6 + k + BLK] * taps[k : k + 1]
    return jax.nn.silu(total).astype(bf16)


def state_kernel(place, x, b, c, xh, bh, ch, xt, bt, ct, cols, xo, bo, co, send, keep):
    xc, bc = conv(x, xh, xt), conv(b, bh, bt)
    xo[...] = xc
    bo[...] = bc
    co[...] = conv(c, ch, ct)
    width = xc.shape[1]
    half = width // 2
    packed = cols[0]
    xf = xc.astype(f32)
    both = []
    for which in (FF, FB):
        scaled = (xf * expand(packed, which, width)).astype(bf16)
        full = lax.dot_general(
            scaled, bc, (((0,), (0,)), ((), ())), preferred_element_type=f32
        )
        both.append((full[:half, :STATE].astype(bf16), full[half:, STATE:].astype(bf16)))

    def put(out):
        for d in range(2):
            out[d, :half], out[d, half:] = both[d]

    turn = pl.program_id(0)
    pl.when(turn < pl.num_programs(0) // 2)(lambda: put(send))
    pl.when(turn >= pl.num_programs(0) // 2)(lambda: put(keep))


def block_kernel(x, b, c, cols, rows, out):
    packed, across = cols[0], rows[0]
    ahead = iota((BLK, BLK), 1) - iota((BLK, BLK), 0)
    lower, upper = ahead < 0, ahead > 0
    lane = iota((BLK, 128), 1)
    scores = [
        lax.dot_general(
            c[:, i * STATE : (i + 1) * STATE],
            b[:, i * STATE : (i + 1) * STATE],
            (((1,), (1,)), ((), ())),
            preferred_element_type=f32,
        )
        for i in range(2)
    ]

    def head(j, pair):
        def col(a):
            return packed[:, a * SLOT + j : a * SLOT + j + 1]

        def row(a):
            return across[a * SLOT + j : a * SLOT + j + 1]

        gaps = jnp.where(lower, col(CF) - row(CF), col(CB) - row(CB))
        rate = jnp.where(lower, row(RF), jnp.where(upper, row(RB), row(RF) + row(RB)))
        weights = (scores[j * 2 // STEP_HEADS] * jnp.exp(gaps) * rate).astype(bf16)
        return jnp.dot(weights, pair, preferred_element_type=f32)

    for k in range(STEP_HEADS // 2):
        at = slice(k * 128, (k + 1) * 128)
        pair = x[:, at]
        out[:, at] = jnp.where(lane < HEAD_DIM, head(2 * k, pair), head(2 * k + 1, pair))


def finish_kernel(place, local, c, cols, mine, theirs, gate, gain, out):
    own = pl.program_id(0) < pl.num_programs(0) // 2
    packed = cols[0]
    width = local.shape[1]
    first = iota((BLK, width), 1) < width // 2
    y = local[...]
    for d, which in enumerate((EF, EB)):
        state = jnp.where(own, mine[d], theirs[d])
        by_group = [
            lax.dot_general(
                c[:, i * STATE : (i + 1) * STATE],
                state,
                (((1,), (1,)), ((), ())),
                preferred_element_type=f32,
            )
            for i in range(2)
        ]
        y = y + jnp.where(first, by_group[0], by_group[1]) * expand(packed, which, width)
    gated = y.astype(bf16).astype(f32) * jax.nn.silu(gate[0].astype(f32))
    same = iota((128, 128), 0) // HEAD_DIM == iota((128, 128), 1) // HEAD_DIM
    ones = jnp.where(same, 1.0 / HEAD_DIM, 0.0).astype(bf16)
    square = gated * gated
    high = square.astype(bf16)
    low = (square - high.astype(f32)).astype(bf16)
    mean = jnp.concatenate(
        [
            jnp.dot(high[:, k : k + 128], ones, preferred_element_type=f32)
            + jnp.dot(low[:, k : k + 128], ones, preferred_element_type=f32)
            for k in range(0, width, 128)
        ],
        axis=1,
    )
    out[0] = (gated * lax.rsqrt(mean + 1e-6) * gain[...].astype(f32)).astype(bf16)


def scan_kernel(uf, ub, decay, of, ob):
    count = uf.shape[0]
    state = jnp.zeros(uf.shape[1:], f32)
    for p in range(count):
        of[p] = state.astype(bf16)
        state = state * decay[0][:, p : p + 1] + uf[p].astype(f32)
    state = jnp.zeros(uf.shape[1:], f32)
    for p in reversed(range(count)):
        ob[p] = state.astype(bf16)
        state = state * decay[1][:, p : p + 1] + ub[p].astype(f32)


def scan_plain(u, decay, reverse):
    def step(state, piece):
        update, factor = piece
        return state * factor[:, None] + update.astype(f32), state.astype(bf16)

    return lax.scan(step, jnp.zeros(u.shape[1:], f32), (u, decay.T), reverse=reverse)[1]


def exchange(uf, ub, totals):
    count = lax.axis_size(ALL)
    heads = totals.shape[1]
    each = uf.shape[0] // count
    everyone = lax.all_gather(totals, ALL)
    mine = lax.axis_index(ALL) * each + jnp.arange(each)
    pick = (mine[:, None] // HEAD_DIM == jnp.arange(heads)[None]).astype(f32)
    decay = jnp.exp(jnp.einsum("rh,pdh->drp", pick, everyone, precision=HIGH))
    uf, ub = (
        lax.all_to_all(u, ALL, split_axis=0, concat_axis=0, tiled=True).reshape(
            count, each, STATE
        )
        for u in (uf, ub)
    )
    if count <= 64:
        shape = jax.ShapeDtypeStruct(uf.shape, bf16)
        sf, sb = pl.pallas_call(scan_kernel, out_shape=(shape, shape))(uf, ub, decay)
    else:
        sf, sb = scan_plain(uf, decay[0], False), scan_plain(ub, decay[1], True)
    return tuple(
        lax.all_to_all(
            s.reshape(count * each, STATE), ALL, split_axis=0, concat_axis=0, tiled=True
        )
        for s in (sf, sb)
    )


def pair_kernel(place, mine, theirs, own, par, send, keep):
    early, fwd = place[0] == 0, place[1] == 1
    e_own, e_par = jnp.exp(own[...]), jnp.exp(par[...])
    scale_mine = (jnp.where(early, e_par[0], 1.0), jnp.where(early, 1.0, e_par[1]))
    scale_theirs = (jnp.where(early, 1.0, e_own[0]), jnp.where(early, e_own[1], 1.0))
    for h in range(own.shape[1]):
        at = slice(h * HEAD_DIM, (h + 1) * HEAD_DIM)
        f, b = (
            mine[d, at].astype(f32) * scale_mine[d][h : h + 1]
            + theirs[d, at].astype(f32) * scale_theirs[d][h : h + 1]
            for d in range(2)
        )
        keep[at] = jnp.where(fwd, f, b).astype(bf16)
        send[at] = jnp.where(fwd, b, f).astype(bf16)


def segment_kernel(place, keep, got, pair, xpair, out):
    fwd = place[1] == 1
    here = jnp.where(fwd, pair[0], pair[1])
    there = jnp.where(fwd, xpair[0], xpair[1])
    factor, total = jnp.exp(here), jnp.exp(here + there)
    high = total.astype(bf16)
    middle = (total - high.astype(f32)).astype(bf16)
    lowest = (total - high.astype(f32) - middle.astype(f32)).astype(bf16)
    parts = [part.astype(f32) for part in (high, middle, lowest)]
    chunks = out.shape[0]
    each = pair.shape[1] // chunks
    rows = each * HEAD_DIM
    for j in range(chunks):
        lines = []
        for i in range(each):
            h = j * each + i
            at = slice(h * HEAD_DIM, (h + 1) * HEAD_DIM)
            new = keep[at].astype(f32) + got[at].astype(f32) * factor[h : h + 1]
            out[j, i * HEAD_DIM : (i + 1) * HEAD_DIM] = new.astype(bf16)
            lines += [part[h : h + 1] for part in parts]
        lines.append(jnp.zeros((out.shape[1] - rows - len(lines), STATE), f32))
        out[j, rows:] = jnp.concatenate(lines, axis=0).astype(bf16)


def carry_kernel(place, v, out):
    fwd = place[1] == 1
    count, rows = out.shape[:2]
    each = rows // HEAD_DIM
    state = [jnp.zeros((HEAD_DIM, STATE), f32)] * each
    for i in range(count):
        q = jnp.where(fwd, i, count - 1 - i)
        piece = v[q].astype(f32)
        lines = piece[rows:]
        for h in range(each):
            at = slice(h * HEAD_DIM, (h + 1) * HEAD_DIM)
            out[q, at] = state[h].astype(bf16)
            factor = lines[3 * h : 3 * h + 1] + lines[3 * h + 1 : 3 * h + 2]
            factor = factor + lines[3 * h + 2 : 3 * h + 3]
            state[h] = state[h] * factor + piece[at]


def enter_kernel(place, entry, other, got, mine, theirs, own, par, xpair, keep, send):
    early, fwd = place[0] == 0, place[1] == 1
    e_own, e_par = jnp.exp(own[...]), jnp.exp(par[...])
    past = jnp.exp(jnp.where(fwd, xpair[0], xpair[1]))
    for h in range(own.shape[1]):
        at = slice(h * HEAD_DIM, (h + 1) * HEAD_DIM)
        line = slice(h, h + 1)
        near = entry[at].astype(f32) * past[line] + got[at].astype(f32)
        far = other[at].astype(f32)
        f, b = jnp.where(fwd, near, far), jnp.where(fwd, far, near)
        f_mine = f * e_par[0, line] + theirs[0, at].astype(f32)
        b_mine = b * e_par[1, line] + theirs[1, at].astype(f32)
        f_theirs = f * e_own[0, line] + mine[0, at].astype(f32)
        b_theirs = b * e_own[1, line] + mine[1, at].astype(f32)
        keep[0, at] = jnp.where(early, f, f_mine).astype(bf16)
        keep[1, at] = jnp.where(early, b_mine, b).astype(bf16)
        send[0, at] = jnp.where(early, f_theirs, f).astype(bf16)
        send[1, at] = jnp.where(early, b, b_theirs).astype(bf16)


def swap(a, bit):
    wide, deep = lax.axis_size("sp"), lax.axis_size("dp")
    perm = [
        (s * deep + d, (s ^ bit) * deep + d) for s in range(wide) for d in range(deep)
    ]
    return lax.ppermute(a, ("sp", "dp"), perm)


def run(kernel, shapes, place, *args):
    smem = pl.BlockSpec(memory_space=pltpu.SMEM)
    vmem = pl.BlockSpec(memory_space=pltpu.VMEM)
    return pl.pallas_call(
        kernel,
        in_specs=[smem] + [vmem] * len(args),
        out_shape=[jax.ShapeDtypeStruct(shape, bf16) for shape in shapes],
    )(place, *args)


def exchange_tree(send, keep, logs, place, block):
    deep = lax.axis_size("dp")
    half = logs.shape[1] // 2
    whole_par = swap(logs, 1)
    whole_pair = logs + whole_par
    whole_xpair = swap(whole_pair, 2)
    own, par, pair, xpair = (
        lax.dynamic_slice_in_dim(a, place[0] * half, half, axis=1)
        for a in (logs, whole_par, whole_pair, whole_xpair)
    )
    theirs = swap(send, 1)
    rows = keep.shape[1:]
    across, stay = run(pair_kernel, (rows, rows), place, keep, theirs, own, par)
    y, got = lax.optimization_barrier((block(), swap(across, 2)))
    each = rows[0] // deep
    (packed,) = run(segment_kernel, ((deep, each + 16, STATE),), place, stay, got, pair, xpair)
    packed = lax.all_to_all(packed, "dp", split_axis=0, concat_axis=0)
    (entry,) = run(carry_kernel, ((deep, each, STATE),), place, packed)
    entry = lax.all_to_all(entry, "dp", split_axis=0, concat_axis=0).reshape(rows)
    other = swap(entry, 2)
    mine, back = run(
        enter_kernel, (keep.shape,) * 2, place, entry, other, got, keep, theirs, own, par, xpair
    )
    return mine, swap(back, 1), y


def local(x, b, c, gate, ahead, back, fade, x_taps, b_taps, c_taps, offsets, exponents, gain):
    tokens, x_width = x.shape[1:]
    b_width = b.shape[2]
    heads = ahead.shape[2]
    steps = heads // STEP_HEADS
    xs, bs = x_width // steps, b_width // steps
    wide, deep = lax.axis_size("sp"), lax.axis_size("dp")
    order = [s * deep + d for d in range(deep) for s in range(wide)]
    up = list(zip(order[:-1], order[1:]))
    down = [(target, source) for source, target in up]

    bounds = [0]
    for piece in (x_taps, b_taps, c_taps, offsets):
        bounds.append(bounds[-1] + piece.shape[1])
    rows_at = [(1, 16, a.shape[2]) for a in (x, b, c)]
    final = tokens // 16 - 1
    small = (x_taps, b_taps, c_taps, offsets, exponents)
    low, high, mine = pl.pallas_call(
        edge_kernel,
        grid=(1,),
        in_specs=[pl.BlockSpec(shape, lambda i: (0, final, 0)) for shape in rows_at]
        + [pl.BlockSpec(shape, lambda i: (0, 0, 0)) for shape in rows_at]
        + [pl.BlockSpec(a.shape, lambda i: (0, 0)) for a in small],
        out_shape=[
            jax.ShapeDtypeStruct((2, x_width + 2 * b_width), bf16),
            jax.ShapeDtypeStruct((1, x_width + 2 * b_width), bf16),
            jax.ShapeDtypeStruct((x_taps.shape[0], bounds[-1]), f32),
        ],
    )(x, b, c, x, b, c, *small)
    if wide == 4:
        spot = lax.axis_index("sp")
        even, left = spot % 2 == 0, spot < 2
        sent = [swap(mine, bit) for bit in (1, 2, 3)]
        near = [jnp.where(even, mine, sent[0]), jnp.where(even, sent[0], mine)]
        far = [jnp.where(even, sent[1], sent[2]), jnp.where(even, sent[2], sent[1])]
        gathered = jnp.stack(
            [jnp.where(left, u, v) for u, v in zip(near + far, far + near)]
        )
    else:
        gathered = lax.all_gather(mine, "sp")
    low = lax.ppermute(low, ("sp", "dp"), up)
    high = lax.ppermute(high, ("sp", "dp"), down)
    width = low.shape[1]
    halo = jnp.concatenate(
        [jnp.zeros((6, width), bf16), low, high, jnp.zeros((7, width), bf16)], axis=0
    )
    xt, bt, ct = (
        jnp.transpose(gathered[:, :, lo:hi], (1, 0, 2)).reshape(gathered.shape[1], -1)
        for lo, hi in zip(bounds[:-2], bounds[1:-1])
    )
    params = jnp.transpose(gathered[:, :, bounds[-2] :], (0, 2, 1)).reshape(heads, -1)
    cols, rows, totals = pl.pallas_call(
        rates_kernel,
        out_shape=(
            jax.ShapeDtypeStruct((steps, BLK, 128), f32),
            jax.ShapeDtypeStruct((steps, 4 * SLOT, BLK), f32),
            jax.ShapeDtypeStruct((2, heads, 128), f32),
        ),
    )(*(jnp.swapaxes(a, 1, 2) for a in (ahead, back, fade)), params)

    def raw(size):
        return pl.BlockSpec((1, tokens, size), lambda g: (0, 0, g))

    def flat(rows_, size, start=0):
        return pl.BlockSpec((rows_, size), lambda g: (0, start + g))

    def stacked(rows_, size=128):
        return pl.BlockSpec((1, rows_, size), lambda g: (g, 0, 0))

    taps = xt.shape[0]
    params_ = pltpu.CompilerParams(dimension_semantics=("arbitrary",))
    tree = wide == 4 and heads % (2 * deep) == 0 and 3 * heads // (2 * deep) <= 16
    if tree:
        spot = lax.axis_index("sp")
        place = jnp.stack([spot % 2, spot // 2]).astype(jnp.int32)
    else:
        place = jnp.zeros((2,), jnp.int32)
    middle = steps // 2

    def shifted(spec, late):
        index = spec.index_map

        def move(g, place):
            return index((g + middle * jnp.where(late, 1 - place[0], place[0])) % steps)

        return pl.BlockSpec(spec.block_shape, move)

    def sided(first):
        def move(g, place):
            return (0, jnp.minimum(g, middle - 1) if first else jnp.maximum(g - middle, 0), 0)

        return pl.BlockSpec((2, xs, STATE), move)

    def half_call(kernel, ins, in_sides, outs, out_sides, late, shapes):
        return pl.pallas_call(
            kernel,
            grid_spec=pltpu.PrefetchScalarGridSpec(
                num_scalar_prefetch=1,
                grid=(steps,),
                in_specs=[shifted(spec, late) for spec in ins[:in_sides[0]]]
                + [sided(first) for first in in_sides[1]]
                + [shifted(spec, late) for spec in ins[in_sides[0] :]],
                out_specs=[shifted(spec, late) for spec in outs] + [sided(f) for f in out_sides],
            ),
            out_shape=shapes,
            compiler_params=params_,
        )
    xc, bc, cc, send, keep = half_call(
        state_kernel,
        [
            raw(xs),
            raw(bs),
            raw(bs),
            flat(16, xs),
            flat(16, bs, x_width // bs),
            flat(16, bs, (x_width + b_width) // bs),
            flat(taps, xs),
            flat(taps, bs),
            flat(taps, bs),
            stacked(BLK),
        ],
        (10, ()),
        [flat(tokens, xs), flat(tokens, bs), flat(tokens, bs)],
        (True, False),
        True,
        [
            jax.ShapeDtypeStruct((tokens, x_width), bf16),
            jax.ShapeDtypeStruct((tokens, b_width), bf16),
            jax.ShapeDtypeStruct((tokens, b_width), bf16),
            jax.ShapeDtypeStruct((2, x_width // 2, STATE), bf16),
            jax.ShapeDtypeStruct((2, x_width // 2, STATE), bf16),
        ],
    )(place, x, b, c, halo, halo, halo, xt, bt, ct, cols)
    block = lambda: pl.pallas_call(
        block_kernel,
        grid=(steps,),
        in_specs=[
            flat(tokens, xs),
            flat(tokens, bs),
            flat(tokens, bs),
            stacked(BLK),
            stacked(4 * SLOT),
        ],
        out_specs=flat(tokens, xs),
        out_shape=jax.ShapeDtypeStruct((tokens, x_width), f32),
        compiler_params=params_,
    )(xc, bc, cc, cols, rows)
    if tree:
        mine, theirs, y = exchange_tree(send, keep, totals, place, block)
    else:
        y = block()
        uf, ub = (jnp.concatenate([keep[d], send[d]], axis=0) for d in range(2))
        states = jnp.stack(exchange(uf, ub, totals[:, :, 0]))
        mine, theirs = states[:, : x_width // 2], states[:, x_width // 2 :]
    (out,) = half_call(
        finish_kernel,
        [flat(tokens, xs), flat(tokens, bs), stacked(BLK), raw(xs), flat(1, xs)],
        (3, (True, False)),
        [raw(xs)],
        (),
        False,
        [jax.ShapeDtypeStruct(x.shape, bf16)],
    )(place, y, cc, cols, mine, theirs, gate, gain[None])
    return out


def solution(mesh):
    token = P("dp", "sp", None)
    placed = (token,) * 7 + (P(None, "sp"),) * 5 + (P(),)
    return jax.shard_map(local, mesh=mesh, in_specs=placed, out_specs=token, check_vma=False)
```
